32 devices in a mesh: kv: 8 (over z, y), tp: 4 (over x, core).
Axes of the slice: x: 2, y: 2, z: 4, core: 2. Of those that a mesh axis runs over, the one named last changes fastest.
Arguments:
- tokens: bfloat16 [1024, 4096], P(None, 'kv'), may hold values from -6 to 6
- norm_gain: float32 [4096], replicated, may hold values from 0.1 to 1.9
- query_weight: bfloat16 [4096, 2048], P('kv', 'tp'), may hold values from -0.09375 to 0.09375
- key_weight: bfloat16 [4096, 2048], P('kv', 'tp'), may hold values from -0.09375 to 0.09375
- value_weight: bfloat16 [4096, 4096], P('kv', 'tp'), may hold values from -0.09375 to 0.09375
- outgate_weight: bfloat16 [4096, 4096], P('kv', 'tp'), may hold values from -0.09375 to 0.09375
- gate_weight: bfloat16 [4096, 32], P('kv'), may hold values from -0.09375 to 0.09375
- forget_bias: float32 [16], replicated, may hold values from -1 to 5
- head_gain: float32 [4096], P('tp'), may hold values from 0.1 to 1.9
- output_weight: bfloat16 [4096, 4096], P('tp', 'kv'), may hold values from -0.09375 to 0.09375
- state_matrix: float32 [256, 16, 128, 256], P('kv', 'tp'), may hold values from -6 to 6
- state_normal: float32 [256, 16, 128], P('kv', 'tp'), may hold values from -6 to 6
- state_stable: float32 [256, 16], P('kv', 'tp'), may hold values from -3 to 3
- prior_keys: bfloat16 [256, 4, 2048], P('kv', None, 'tp'), may hold values from -0.59765625 to 0.59765625
- prior_values: bfloat16 [256, 4, 4096], P('kv', None, 'tp'), may hold values from -6 to 6
- prior_ingate: float32 [256, 4, 16], P('kv', None, 'tp'), may hold values from -4 to 4
- prior_forget: float32 [256, 4, 16], P('kv', None, 'tp'), may hold values from -2 to -0.02
- accepted: int32 [256], P('kv'), may hold values from 0 to 4
- parents: int32 [256, 4], P('kv'), may hold values from -1 to 2, as said below
Outputs:
- layer_out: bfloat16 [1024, 4096], P('tp', 'kv')
- new_matrix: float32 [256, 16, 128, 256], P('kv', 'tp')
- new_normal: float32 [256, 16, 128], P('kv', 'tp')
- new_stable: float32 [256, 16], P('kv', 'tp')
The draws below stay inside these ranges and needn't reach their ends.
Inputs may be any that keep to these rules, and one draw needn't show every extreme that they name: parents of proposal t lie in -1 to t - 1; the first proposal's parent is -1; in some sequence each proposal's parent is the one before it.
All inputs are finite; a program needn't handle non-finite values.
Results may differ from the reference program's by a relative error of at most 0.0089.
Values may be sent and summed in bfloat16 or wider, within the bound.
A program may use at most 128 MiB of HBM per device.

```python
import jax
import jax.numpy as jnp
from jax import lax

D = 4096
HEADS = 16
DQK = 128
DV = 256
PROP = 4
SEQS = 256
TOKENS = 1024


def draw_parents(key, part):
    random_ints = jax.random.randint(key, (SEQS, PROP), 0, 1 << 20)
    position = jnp.arange(PROP, dtype=jnp.int32)[None, :]
    chosen = random_ints % jnp.maximum(position, 1)
    leading = jnp.arange(SEQS, dtype=jnp.int32)[:, None] == 0
    chosen = jnp.where(leading, position - 1, chosen)
    return jnp.where(position == 0, -1, chosen).astype(jnp.int32)


def set_ends(entries, rng, least, top_value):
    dims = entries.shape
    place = [jax.random.randint(jax.random.fold_in(rng, axis), (), 0, dims[axis]) for axis in range(len(dims))]
    entries = entries.at[tuple(place)].set(least)
    longest = dims.index(max(dims))
    place[longest] = (place[longest] + 1) % dims[longest]
    return entries.at[tuple(place)].set(top_value)


def block_scale(rng, shape, shards, least, largest):
    def one(axis_at, parts):
        steps = jax.random.uniform(jax.random.fold_in(jax.random.fold_in(rng, 6), axis_at), (parts,), jnp.float32, least / len(shards), largest / len(shards))
        return jnp.repeat(jnp.exp(steps), shape[axis_at] // parts).reshape((-1,) + (1,) * (len(shape) - axis_at - 1))

    factor_of = one(*shards[0])
    for cut in shards[1:]:
        factor_of = factor_of * one(*cut)
    return factor_of


def centred(rng, dims, scale, most, shards=(), kind=jnp.bfloat16):
    loudness = block_scale(rng, dims, shards, -0.22, 0.18) if shards else 1.0
    array = jax.random.normal(rng, dims, jnp.float32) * scale * loudness
    return jnp.minimum(jnp.maximum(array, -most), most).astype(kind)


def setup_inputs(seed: int = 0) -> dict:
    keys = jax.random.split(jax.random.key(seed), 20)
    return {
        "tokens": centred(keys[0], (TOKENS, D), 1.0, 6.0, ((1, 8),)),
        "norm_gain": jnp.clip(1.0 + 0.18 * jax.random.normal(keys[1], (D,), jnp.float32), 0.1, 1.9),
        "query_weight": centred(keys[2], (D, HEADS * DQK), D ** -0.5, 0.09375, ((0, 8), (1, 4))),
        "key_weight": centred(keys[3], (D, HEADS * DQK), D ** -0.5, 0.09375, ((0, 8), (1, 4))),
        "value_weight": centred(keys[4], (D, HEADS * DV), D ** -0.5, 0.09375, ((0, 8), (1, 4))),
        "outgate_weight": centred(keys[5], (D, HEADS * DV), D ** -0.5, 0.09375, ((0, 8), (1, 4))),
        "gate_weight": centred(keys[6], (D, 2 * HEADS), D ** -0.5, 0.09375, ((0, 8),)),
        "forget_bias": jnp.clip(jax.random.uniform(keys[7], (HEADS,), jnp.float32, -1.0, 5.0), -1.0, 5.0),
        "head_gain": jnp.clip(1.0 + 0.18 * jax.random.normal(keys[8], (HEADS * DV,), jnp.float32), 0.1, 1.9),
        "output_weight": centred(keys[9], (HEADS * DV, D), (HEADS * DV) ** -0.5, 0.09375, ((0, 4), (1, 8))),
        "state_matrix": centred(keys[10], (SEQS, HEADS, DQK, DV), 1.0, 6.0, ((0, 8), (1, 4)), jnp.float32),
        "state_normal": centred(keys[11], (SEQS, HEADS, DQK), 1.0, 6.0, ((0, 8), (1, 4)), jnp.float32),
        "state_stable": centred(keys[12], (SEQS, HEADS), 1.0, 3.0, ((0, 8), (1, 4)), jnp.float32),
        "prior_keys": centred(keys[13], (SEQS, PROP, HEADS * DQK), 0.09, 0.59765625, ((0, 8), (2, 4))),
        "prior_values": centred(keys[14], (SEQS, PROP, HEADS * DV), 1.0, 6.0, ((0, 8), (2, 4))),
        "prior_ingate": centred(keys[15], (SEQS, PROP, HEADS), 1.0, 4.0, ((0, 8), (2, 4)), jnp.float32),
        "prior_forget": jnp.clip(-2.0 + 1.98 * jax.random.uniform(keys[16], (SEQS, PROP, HEADS), jnp.float32) ** block_scale(keys[16], (SEQS, PROP, HEADS), ((0, 8), (2, 4)), -0.2, 0.2), -2.0, -0.02),
        "accepted": set_ends(jax.random.randint(keys[17], (SEQS,), 0, PROP + 1), jax.random.fold_in(keys[17], 1), 0, PROP).astype(jnp.int32),
        "parents": draw_parents(jax.random.fold_in(keys[19], 71), 0),
    }


def ancestry(parents):
    count = parents.shape[1]
    index = jnp.arange(count, dtype=jnp.int32)
    current = jnp.broadcast_to(index[None, :], parents.shape).astype(jnp.int32)
    table = jnp.broadcast_to((index[:, None] == index[None, :]).astype(jnp.float32), (parents.shape[0], count, count))
    for repeat in range(count - 1):
        looked = jnp.take_along_axis(parents, jnp.maximum(current, 0), axis=1)
        current = jnp.where(current >= 0, looked, -1).astype(jnp.int32)
        table = table + (current[:, :, None] == index[None, None, :]).astype(jnp.float32)
    return table

def commit(matrix, normal, stable, prior_k, prior_v, prior_i, prior_f, accepted):
    count = prior_k.shape[1]
    live = (jnp.arange(count, dtype=jnp.int32)[None, :] < accepted[:, None])[:, :, None]
    forget_live = jnp.where(live, prior_f, 0.0)
    cumul = jnp.cumsum(forget_live, axis=1)
    total = cumul[:, -1]
    weight_log = jnp.where(live, total[:, None, :] - cumul + prior_i, -jnp.inf)
    new_stable = jnp.maximum(total + stable, lax.optimization_barrier(jnp.max(weight_log, axis=1)))
    weights = jnp.exp(weight_log - new_stable[:, None, :])
    decay = jnp.exp(total + stable - new_stable)
    hp = lax.Precision.HIGHEST
    new_matrix = decay[:, :, None, None] * matrix + jnp.einsum('sph,sphd,sphv->shdv', weights, prior_k, prior_v, precision=hp)
    new_normal = decay[:, :, None] * normal + jnp.einsum('sph,sphd->shd', weights, prior_k, precision=hp)
    return (new_matrix, new_normal, new_stable)

def tree_read(query, key_rows, value_rows, ingate, logforget, table, matrix, normal, stable):
    hp = lax.Precision.HIGHEST
    path_sum = jnp.einsum('sta,sah->sth', table, logforget, precision=hp)
    dlog = path_sum[:, :, None, :] - path_sum[:, None, :, :] + ingate[:, None, :, :]
    dlog = jnp.where(table[:, :, :, None] > 0.5, dlog, -jnp.inf)
    carried = path_sum + stable[:, None, :]
    top = jnp.maximum(carried, lax.optimization_barrier(jnp.max(dlog, axis=2)))
    scores = jnp.einsum('sthd,sahd->stah', query, key_rows, precision=hp) * jnp.exp(dlog - top[:, :, None, :])
    factor = jnp.exp(carried - top)
    numer = jnp.einsum('stah,sahv->sthv', scores, value_rows, precision=hp) + factor[..., None] * jnp.einsum('sthd,shdv->sthv', query, matrix, precision=hp)
    denom = lax.optimization_barrier(jnp.sum(scores, axis=2)) + factor * jnp.einsum('sthd,shd->sth', query, normal, precision=hp)
    return numer / jnp.maximum(jnp.abs(denom), jnp.exp(-top))[..., None]

def reference(tokens, norm_gain, query_weight, key_weight, value_weight, outgate_weight, gate_weight, forget_bias, head_gain, output_weight, state_matrix, state_normal, state_stable, prior_keys, prior_values, prior_ingate, prior_forget, accepted, parents):
    f32 = jnp.float32
    xfloat = tokens.astype(f32)
    scale = lax.rsqrt(lax.optimization_barrier(jnp.sum(xfloat * xfloat, axis=-1, keepdims=True)) / D + 1e-06)
    normed = (xfloat * norm_gain).astype(jnp.bfloat16)
    query = scale * jnp.dot(normed, query_weight, preferred_element_type=f32)
    key_rows = scale * jnp.dot(normed, key_weight, preferred_element_type=f32) / jnp.sqrt(jnp.float32(DQK))
    value_rows = scale * jnp.dot(normed, value_weight, preferred_element_type=f32)
    outgate = scale * jnp.dot(normed, outgate_weight, preferred_element_type=f32)
    gates = scale * jnp.dot(normed, gate_weight, preferred_element_type=f32)
    ingate = gates[:, :HEADS].reshape(SEQS, PROP, HEADS)
    logforget = jax.nn.log_sigmoid(gates[:, HEADS:] + forget_bias).reshape(SEQS, PROP, HEADS)
    new_matrix, new_normal, new_stable = commit(state_matrix, state_normal, state_stable, prior_keys.astype(f32).reshape(SEQS, PROP, HEADS, DQK), prior_values.astype(f32).reshape(SEQS, PROP, HEADS, DV), prior_ingate, prior_forget, accepted)
    table = ancestry(parents)
    read = tree_read(query.reshape(SEQS, PROP, HEADS, DQK), key_rows.reshape(SEQS, PROP, HEADS, DQK), value_rows.reshape(SEQS, PROP, HEADS, DV), ingate, logforget, table, new_matrix, new_normal, new_stable)
    normer = lax.rsqrt(lax.optimization_barrier(jnp.mean(read * read, axis=-1, keepdims=True)) + 1e-06)
    hidden = read * normer * head_gain.reshape(HEADS, DV) * jax.nn.sigmoid(outgate.reshape(SEQS, PROP, HEADS, DV))
    hidden = hidden.reshape(TOKENS, HEADS * DV).astype(jnp.bfloat16)
    layer_out = jnp.dot(hidden, output_weight, preferred_element_type=f32).astype(jnp.bfloat16)
    return (layer_out, new_matrix, new_normal, new_stable)
```

```python
import functools

import jax
import jax.numpy as jnp
from jax import lax
from jax.experimental import pallas as pl
from jax.experimental.pallas import tpu as pltpu
from jax.sharding import PartitionSpec as P

D = 4096
HEADS = 16
DQK = 128
DV = 256
PROP = 4
LANES = 128
HALF = 64
NEG = -1e30
F32 = jnp.float32
BF16 = jnp.bfloat16
HP = lax.Precision.HIGHEST


def ancestry(parents):
    count = parents.shape[1]
    index = jnp.arange(count, dtype=jnp.int32)
    current = jnp.broadcast_to(index[None, :], parents.shape)
    table = jnp.broadcast_to(
        (index[:, None] == index[None, :]).astype(F32), (parents.shape[0], count, count)
    )
    for repeat in range(count - 1):
        hit = current[:, :, None] == index[None, None, :]
        looked = jnp.sum(jnp.where(hit, parents[:, None, :], 0), axis=2)
        current = jnp.where(current >= 0, looked, -1)
        table = table + (current[:, :, None] == index[None, None, :]).astype(F32)
    return table


def split_halves(full):
    lane = lax.broadcasted_iota(jnp.int32, full.shape, full.ndim - 1)
    lead = full.astype(BF16)
    rest = (full - lead.astype(F32)).astype(BF16)
    return jnp.where(lane < HALF, lead.astype(F32), rest.astype(F32)).astype(BF16)


def proj_kernel(with_gates, sq_lane, *refs):
    idx_ref, tok_ref, gain_ref = refs[:3]
    weights = refs[3:-1]
    out_ref = refs[-1]
    x = tok_ref[...].astype(F32)
    normed = (x * gain_ref[...]).astype(BF16)
    at = 0
    for n, w_ref in enumerate(weights):
        width = w_ref.shape[1]
        prod = jnp.dot(normed, w_ref[...], preferred_element_type=F32)
        if with_gates and n == 0:
            squares = jnp.sum(x * x, axis=1, keepdims=True)
            lane = lax.broadcasted_iota(jnp.int32, prod.shape, 1)
            full = jnp.where(lax.rem(lane, HALF) == sq_lane, squares, prod)
            out_ref[0, :, at : at + width] = split_halves(full)
        else:
            out_ref[0, :, at : at + width] = prod.astype(BF16)
        at += width


def project(idx, tokens, gain, weights, rows, with_gates, sq_lane):
    blocks = idx.shape[0]
    depth = tokens.shape[1]
    total = sum(w.shape[1] for w in weights)
    return pl.pallas_call(
        functools.partial(proj_kernel, with_gates, sq_lane),
        out_shape=jax.ShapeDtypeStruct((blocks, rows, total), BF16),
        grid_spec=pltpu.PrefetchScalarGridSpec(
            num_scalar_prefetch=1,
            grid=(blocks,),
            in_specs=[
                pl.BlockSpec((rows, depth), lambda i, idx: (idx[i], 0)),
                pl.BlockSpec((1, depth), lambda i, idx: (0, 0)),
            ]
            + [pl.BlockSpec(w.shape, lambda i, idx: (0, 0)) for w in weights],
            out_specs=pl.BlockSpec((1, rows, total), lambda i, idx: (i, 0, 0)),
        ),
        cost_estimate=pl.CostEstimate(
            flops=2 * blocks * rows * depth * total,
            bytes_accessed=2 * depth * total + 2 * blocks * rows * total,
            transcendentals=0,
        ),
        name="project",
    )(idx, tokens, gain, *weights)


def combine_kernel(count, with_gates, *refs):
    ins = refs[:count]
    outs = refs[count:]
    for b, out_ref in enumerate(outs):
        acc = ins[0][b].astype(F32)
        for other in ins[1:]:
            acc = acc + other[b].astype(F32)
        if with_gates:
            gates = acc[:, :LANES]
            gates = gates + pltpu.roll(gates, HALF, 1)
            out_ref[:, :LANES] = split_halves(gates)
            out_ref[:, LANES:] = acc[:, LANES:].astype(BF16)
        else:
            out_ref[...] = acc.astype(BF16)


def combine(parts, with_gates):
    blocks, rows, width = parts[0].shape
    vmem = pl.BlockSpec(memory_space=pltpu.VMEM)
    return pl.pallas_call(
        functools.partial(combine_kernel, len(parts), with_gates),
        out_shape=[jax.ShapeDtypeStruct((rows, width), BF16)] * blocks,
        in_specs=[vmem] * len(parts),
        out_specs=[vmem] * blocks,
        cost_estimate=pl.CostEstimate(
            flops=0,
            bytes_accessed=2 * (len(parts) + 1) * blocks * rows * width,
            transcendentals=0,
        ),
        name="combine",
    )(*parts)


def commit_kernel(seqs, heads, decay_ref, m_ref, k_ref, v_ref, w_ref, out_ref, low_ref):
    step = pl.program_id(0)
    rows = seqs * PROP
    row_seq = lax.broadcasted_iota(jnp.int32, (rows, 1), 0) // PROP
    for h in range(heads):
        keys = k_ref[:, h * DQK : (h + 1) * DQK].astype(F32)
        vals = v_ref[:, h * DV : (h + 1) * DV].astype(F32) * w_ref[:, h : h + 1]
        lead = vals.astype(BF16)
        rest = (vals - lead.astype(F32)).astype(BF16)
        both = jnp.concatenate([lead, rest], axis=0)
        for s in range(seqs):
            own = jnp.where(row_seq == s, keys, 0.0).astype(BF16)
            added = lax.dot_general(
                jnp.concatenate([own, own], axis=0),
                both,
                (((0,), (0,)), ((), ())),
                preferred_element_type=F32,
            )
            new = decay_ref[step * seqs + s, h] * m_ref[s, h] + added
            out_ref[s, h] = new
            low_ref[s, h] = new.astype(BF16)


def commit_matrix(decay, matrix, keys, values, weights, seqs):
    total, heads, _, _ = matrix.shape
    rows = seqs * PROP
    block = pl.BlockSpec((seqs, heads, DQK, DV), lambda i: (i, 0, 0, 0))
    return pl.pallas_call(
        functools.partial(commit_kernel, seqs, heads),
        grid=(total // seqs,),
        out_shape=[
            jax.ShapeDtypeStruct(matrix.shape, F32),
            jax.ShapeDtypeStruct(matrix.shape, BF16),
        ],
        in_specs=[
            pl.BlockSpec(memory_space=pltpu.SMEM),
            block,
            pl.BlockSpec((rows, heads * DQK), lambda i: (i, 0)),
            pl.BlockSpec((rows, heads * DV), lambda i: (i, 0)),
            pl.BlockSpec((rows, LANES), lambda i: (i, 0)),
        ],
        out_specs=[block, block],
        cost_estimate=pl.CostEstimate(
            flops=2 * matrix.size * 8, bytes_accessed=matrix.size * 10, transcendentals=0
        ),
        name="commit",
    )(decay, matrix, keys, values, weights)


def read_kernel(heads, ny, nz, *refs):
    first = refs[:nz]
    second = refs[nz : nz + ny]
    m_ref, table_ref, stable_ref, normal_ref, bias_ref, gain_ref, out_ref = refs[nz + ny :]
    rows = out_ref.shape[0]
    one = first[0][...].astype(F32)
    for r in first[1:]:
        one = one + r[...].astype(F32)
    two = second[0][...].astype(F32)
    for r in second[1:]:
        two = two + r[...].astype(F32)
    gates = one[:, :LANES]
    gates = gates + pltpu.roll(gates, HALF, 1)
    scale = lax.rsqrt(gates[:, 2 * heads : 2 * heads + 1] * (1.0 / D) + 1e-06)
    gates = scale * gates
    x = gates + bias_ref[...]
    logforget = jnp.minimum(x, 0.0) - jnp.log1p(jnp.exp(-jnp.abs(x)))
    table = table_ref[...]
    path = jnp.dot(table, logforget, precision=HP, preferred_element_type=F32)
    lifted = pltpu.roll(gates, heads, 1) - path
    pick = (
        lax.broadcasted_iota(jnp.int32, (8, LANES), 1)
        == lax.broadcasted_iota(jnp.int32, (8, LANES), 0) + heads
    ).astype(F32)
    flat = lax.dot_general(
        pick, lifted, (((1,), (1,)), ((), ())), precision=HP, preferred_element_type=F32
    )
    carried_all = path + stable_ref[...]
    row16 = lax.broadcasted_iota(jnp.int32, (16, 1), 0) // PROP
    key_scale = scale / jnp.sqrt(jnp.float32(DQK))
    at_value = LANES + heads * DQK
    at_gate = heads * DQK
    for h in range(heads):
        query = scale * one[:, LANES + h * DQK : LANES + (h + 1) * DQK]
        value = scale * one[:, at_value + h * DV : at_value + (h + 1) * DV]
        key = key_scale * two[:, h * DQK : (h + 1) * DQK]
        outgate = scale * two[:, at_gate + h * DV : at_gate + (h + 1) * DV]
        dlog = path[:, heads + h : heads + h + 1] + flat[h : h + 1, :]
        dlog = jnp.where(table > 0.5, dlog, NEG)
        carried = carried_all[:, heads + h : heads + h + 1]
        top = jnp.maximum(carried, jnp.max(dlog, axis=1, keepdims=True))
        scores = lax.dot_general(
            query, key, (((1,), (1,)), ((), ())), precision=HP, preferred_element_type=F32
        ) * jnp.exp(dlog - top)
        factor = jnp.exp(carried - top)
        low = query.astype(BF16)
        pieces = []
        for g in range(rows // 16):
            part = low[g * 16 : (g + 1) * 16]
            got = None
            for j in range(16 // PROP):
                res = jnp.dot(
                    part, m_ref[g * (16 // PROP) + j, h], preferred_element_type=F32
                )
                got = res if got is None else jnp.where(row16 == j, res, got)
            pieces.append(got)
        from_state = jnp.concatenate(pieces, axis=0)
        numer = (
            jnp.dot(scores, value, precision=HP, preferred_element_type=F32)
            + factor * from_state
        )
        denom = jnp.sum(scores, axis=1, keepdims=True) + factor * jnp.sum(
            query * normal_ref[:, h * DQK : (h + 1) * DQK], axis=1, keepdims=True
        )
        read = numer / jnp.maximum(jnp.abs(denom), jnp.exp(-top))
        normer = lax.rsqrt(jnp.mean(read * read, axis=1, keepdims=True) + 1e-06)
        hidden = (
            read
            * normer
            * gain_ref[:, h * DV : (h + 1) * DV]
            * (1.0 / (1.0 + jnp.exp(-outgate)))
        )
        out_ref[:, h * DV : (h + 1) * DV] = hidden.astype(BF16)


def tree_read(first, second, matrix, table, stable, normal, bias, gain, rows):
    heads = matrix.shape[1]
    total = first[0].shape[0]
    seqs = rows // PROP

    def by_row(a):
        return pl.BlockSpec((rows, a.shape[1]), lambda i: (i, 0))

    def whole(a):
        return pl.BlockSpec(a.shape, lambda i: (0, 0))

    return pl.pallas_call(
        functools.partial(read_kernel, heads, len(second), len(first)),
        grid=(total // rows,),
        out_shape=jax.ShapeDtypeStruct((total, heads * DV), BF16),
        in_specs=[by_row(a) for a in first]
        + [by_row(a) for a in second]
        + [
            pl.BlockSpec((seqs, heads, DQK, DV), lambda i: (i, 0, 0, 0)),
            pl.BlockSpec((rows, rows), lambda i: (i, 0)),
            by_row(stable),
            by_row(normal),
            whole(bias),
            whole(gain),
        ],
        out_specs=pl.BlockSpec((rows, heads * DV), lambda i: (i, 0)),
        cost_estimate=pl.CostEstimate(
            flops=8 * matrix.size, bytes_accessed=matrix.size * 2, transcendentals=0
        ),
        name="tree_read",
    )(*first, *second, matrix, table, stable, normal, bias, gain)


def per_device(
    kv,
    tp,
    tokens,
    norm_gain,
    query_weight,
    key_weight,
    value_weight,
    outgate_weight,
    gate_weight,
    forget_bias,
    head_gain,
    output_weight,
    state_matrix,
    state_normal,
    state_stable,
    prior_keys,
    prior_values,
    prior_ingate,
    prior_forget,
    accepted,
    parents,
):
    ny = 1 << ((kv.bit_length() - 1) // 2)
    nz = kv // ny
    me = lax.axis_index("kv")
    mine = lax.axis_index("tp")
    z, y = me // ny, lax.rem(me, ny)
    heads = query_weight.shape[1] // DQK
    depth = tokens.shape[1]
    seqs = accepted.shape[0]
    rows = seqs * PROP

    def over_y(a, d):
        return lax.ppermute(
            a, "kv", [(p * ny + q, p * ny + (q + d) % ny) for p in range(nz) for q in range(ny)]
        )

    def over_z(a, d):
        return lax.ppermute(
            a, "kv", [(p * ny + q, (p + d) % nz * ny + q) for p in range(nz) for q in range(ny)]
        )

    own_gain = lax.dynamic_slice_in_dim(norm_gain, me * depth, depth, 0)[None, :]
    head_start = mine * heads
    picked = lax.dynamic_slice_in_dim(
        gate_weight.reshape(depth, 2, HEADS), head_start, heads, 2
    ).reshape(depth, 2 * heads)
    half_gate = jnp.pad(picked, ((0, 0), (0, HALF - 2 * heads)))
    gate_cols = jnp.concatenate([half_gate, half_gate], axis=1)
    y_first = (gate_cols, query_weight, value_weight)
    z_first = (key_weight, outgate_weight)

    def y_part(d):
        zz = lax.rem(z + jnp.arange(nz, dtype=jnp.int32), nz)
        idx = zz * ny + lax.rem(y + d, ny)
        return project(idx, tokens, own_gain, y_first, rows, True, 2 * heads)

    def z_part(d):
        yy = lax.rem(y + jnp.arange(ny, dtype=jnp.int32), ny)
        idx = lax.rem(z + d, nz) * ny + yy
        return project(idx, tokens, own_gain, z_first, rows, False, 0)

    y_got = [over_y(y_part(d), d) for d in range(1, ny)]
    z_got = [over_z(z_part(d), d) for d in range(1, nz)]
    y_own = y_part(0)
    z_own = z_part(0)

    live = (jnp.arange(PROP, dtype=jnp.int32)[None, :] < accepted[:, None])[:, :, None]
    forget_live = jnp.where(live, prior_forget, 0.0)
    cumul = [forget_live[:, 0]]
    for p in range(1, PROP):
        cumul.append(cumul[-1] + forget_live[:, p])
    total = cumul[-1]
    cumul = jnp.stack(cumul, axis=1)
    weight_log = jnp.where(live, total[:, None, :] - cumul + prior_ingate, -jnp.inf)
    new_stable = jnp.maximum(total + state_stable, jnp.max(weight_log, axis=1))
    weights = jnp.exp(weight_log - new_stable[:, None, :])
    decay = jnp.exp(total + state_stable - new_stable)
    new_normal = decay[:, :, None] * state_normal + jnp.sum(
        weights[..., None] * prior_keys.astype(F32).reshape(seqs, PROP, heads, DQK), axis=1
    )
    weight_rows = jnp.pad(weights.reshape(rows, heads), ((0, 0), (0, LANES - heads)))
    new_matrix, low_matrix = commit_matrix(
        decay,
        state_matrix,
        prior_keys.reshape(rows, heads * DQK),
        prior_values.reshape(rows, heads * DV),
        weight_rows,
        4,
    )

    step_rows = 32
    group = step_rows // PROP
    table = ancestry(parents)
    spread = (
        table.reshape(seqs // group, group, PROP, 1, PROP)
        * jnp.eye(group, dtype=F32)[None, :, None, :, None]
    ).reshape(rows, step_rows)
    stable_rows = jnp.pad(
        jnp.repeat(new_stable, PROP, axis=0), ((0, 0), (heads, LANES - 2 * heads))
    )
    normal_rows = jnp.repeat(new_normal.reshape(seqs, heads * DQK), PROP, axis=0)
    bias = jnp.pad(
        lax.dynamic_slice_in_dim(forget_bias, head_start, heads, 0), (heads, LANES - 2 * heads)
    )[None, :]

    y_own, z_own, low_matrix = lax.optimization_barrier((y_own, z_own, low_matrix))
    y_sums = combine([y_own] + y_got, True)
    first = [y_sums[0]] + [over_z(y_sums[d], d) for d in range(1, nz)]
    z_sums = combine([z_own] + z_got, False)
    second = [z_sums[0]] + [over_y(z_sums[d], d) for d in range(1, ny)]

    hidden = tree_read(
        first,
        second,
        low_matrix,
        spread,
        stable_rows,
        normal_rows,
        bias,
        head_gain[None, :],
        step_rows,
    )

    plane = jnp.stack([hidden] + [over_y(hidden, d) for d in range(1, ny)], axis=0)
    blocks = [plane] + [over_z(plane, d) for d in range(1, nz)]
    parts = jnp.stack(
        [
            jnp.dot(
                b.reshape(ny * rows, heads * DV), output_weight, preferred_element_type=F32
            )
            .astype(BF16)
            .reshape(ny, rows, -1)
            for b in blocks
        ]
    ).reshape(kv, rows, -1)
    per = kv // tp

    def chunk(dest):
        out = []
        for j in range(per):
            b = dest * per + j
            dz = lax.rem(z - b // ny + nz, nz)
            dy = lax.rem(y - lax.rem(b, ny) + ny, ny)
            out.append(lax.dynamic_index_in_dim(parts, dz * ny + dy, 0, keepdims=False))
        return jnp.concatenate(out, axis=0)

    acc = chunk(mine).astype(F32)
    for d in range(1, tp):
        got = lax.ppermute(
            chunk(lax.rem(mine + d, tp)), "tp", [(t, (t + d) % tp) for t in range(tp)]
        )
        acc = acc + got.astype(F32)
    return (acc.astype(BF16), new_matrix, new_normal, new_stable)


def solution(mesh):
    placed = (
        P(None, "kv"),
        P(),
        P("kv", "tp"),
        P("kv", "tp"),
        P("kv", "tp"),
        P("kv", "tp"),
        P("kv", None),
        P(),
        P("tp"),
        P("tp", "kv"),
        P("kv", "tp", None, None),
        P("kv", "tp", None),
        P("kv", "tp"),
        P("kv", None, "tp"),
        P("kv", None, "tp"),
        P("kv", None, "tp"),
        P("kv", None, "tp"),
        P("kv"),
        P("kv", None),
    )
    return jax.shard_map(
        functools.partial(per_device, mesh.shape["kv"], mesh.shape["tp"]),
        mesh=mesh,
        in_specs=placed,
        out_specs=(P("tp", "kv"), P("kv", "tp", None, None), P("kv", "tp", None), P("kv", "tp")),
        check_vma=False,
    )
```
